256 devices in a mesh: ep: 16 (over y, x), tp: 16 (over z, core).
Axes of the slice: x: 4, y: 4, z: 8, core: 2. Of those that a mesh axis runs over, the one named last changes fastest.
Arguments:
- queries: bfloat16 [16384, 1024], P('ep', 'tp'), may hold values from -30 to 30
- key_vectors: bfloat16 [16384, 1024], P('ep', 'tp'), may hold values from -30 to 30
- value_vectors: bfloat16 [16384, 1024], P('ep', 'tp'), may hold values from -9 to 9
- cumulative_gate: float32 [16384, 16], P('ep', 'tp'), as said below
- out_weight: bfloat16 [1024, 2048], P('tp'), may hold values from -0.1875 to 0.1875
- expert_tokens: bfloat16 [24576, 2048], P(('ep', 'tp')), may hold values from -6 to 6
- norm_gain: float32 [2048], replicated, may hold values from 0.1 to 1.9
- gate_weight: bfloat16 [16, 2048, 2048], P('ep', None, 'tp'), may hold values from -0.375 to 0.375
- up_weight: bfloat16 [16, 2048, 2048], P('ep', None, 'tp'), may hold values from -0.375 to 0.375
- down_weight: bfloat16 [16, 2048, 2048], P('ep', 'tp'), may hold values from -0.015625 to 0.015625
- expert_choice: int32 [24576, 2], P(('ep', 'tp')), may hold values from 0 to 15, all different within a row; in each aligned block of 96 rows (0 to 95, 96 to 191, ...) at most 13 rows name the same one
- route_weights: float32 [24576, 2], P(('ep', 'tp')), may hold values from 0.2 to 1
Outputs:
- mixer_output: bfloat16 [16384, 2048], P(('ep', 'tp'))
- expert_output: bfloat16 [24576, 2048], P(('ep', 'tp'))
The draws below stay inside these ranges and needn't reach their ends.
Inputs may be any that keep to these rules, and one draw needn't show every extreme that they name: `cumulative_gate`: each head's values never rise from one position to the next. `expert_choice`: each row names 2 different experts; within the rows of one device no expert is named more than 13 times, and in some of them one expert exactly 13 times.
All inputs are finite; a program needn't handle non-finite values.
Results may differ from the reference program's by a relative error of at most 0.019.
Values may be sent and summed in bfloat16 or wider, within the bound.
No kernel may reach another device: no remote copies, remote signals or barrier semaphores. Data moves between devices by JAX's collectives and lax.ppermute only.
A program may use at most 128 MiB of HBM per device.

```python
import math
import jax
import jax.numpy as jnp
import numpy as np
from jax import lax

D = 2048
HEAD_DIM = 64
HEAD_COUNT = 16
FF = 2048
EXPERTS = 16
TOPK = 2
TOK_DEV = 96
CAP = 13
ROWS = 1024
TOKEN_POSITIONS = 16384
EXP_TOKENS = 24576
N_TP = 16


def paired_vectors(key):
    full_width = HEAD_COUNT * HEAD_DIM
    query_key = jax.random.fold_in(key, 101)
    vector_key = jax.random.fold_in(key, 102)
    queries = jnp.clip(jax.random.normal(query_key, (TOKEN_POSITIONS, full_width), jnp.float32), -6.0, 6.0)
    vectors = jnp.clip(jax.random.normal(vector_key, (TOKEN_POSITIONS, full_width), jnp.float32), -6.0, 6.0)
    return (queries, vectors)


def draw_queries(key, part):
    return paired_vectors(key)[0].astype(jnp.bfloat16)


def draw_key_vectors(key, part):
    return paired_vectors(key)[1].astype(jnp.bfloat16)


def draw_cumulative_gate(key, part):
    fast_share = 0.5
    head_draw = jax.random.uniform(jax.random.fold_in(key, 201), (HEAD_COUNT,), jnp.float32)
    fast_rate = jnp.exp(jax.random.uniform(jax.random.fold_in(key, 202), (HEAD_COUNT,), jnp.float32, math.log(0.012), math.log(0.035)))
    slow_rate = jnp.exp(jax.random.uniform(jax.random.fold_in(key, 203), (HEAD_COUNT,), jnp.float32, math.log(0.1), math.log(0.5))) / TOKEN_POSITIONS
    head_rate = jnp.where(head_draw < fast_share, fast_rate, slow_rate)
    block_count = TOKEN_POSITIONS // ROWS
    block_factor = jnp.exp(jax.random.uniform(jax.random.fold_in(key, 204), (block_count,), jnp.float32, math.log(0.4), math.log(2.5)))
    position_factor = jnp.repeat(block_factor, ROWS)
    roughness = jax.random.uniform(jax.random.fold_in(key, 205), (TOKEN_POSITIONS, HEAD_COUNT), jnp.float32, 0.3, 1.7)
    logarithm_gate = -head_rate[None, :] * position_factor[:, None] * roughness
    spike_rows = jax.random.randint(jax.random.fold_in(key, 206), (3,), 0, TOKEN_POSITIONS)
    spike_loss = jax.random.uniform(jax.random.fold_in(key, 207), (3, HEAD_COUNT), jnp.float32, 0.2, 0.4)
    logarithm_gate = logarithm_gate.at[spike_rows].add(jnp.log1p(-spike_loss))
    return jnp.cumsum(logarithm_gate, axis=0)


def block_levels(key, dims, cuts, smallest, high):
    loudness = 1.0
    for position, shards_of in cuts:
        draws = jax.random.uniform(jax.random.fold_in(jax.random.fold_in(key, 6), position), (shards_of,), jnp.float32, smallest / len(cuts), high / len(cuts))
        loudness = loudness * jnp.repeat(jnp.exp(draws), dims[position] // shards_of).reshape((-1,) + (1,) * (len(dims) - 1 - position))
    return loudness


def deal_out(stream_key, own, number, rows, amount, top, limit, lean):
    order = jax.random.permutation(stream_key, amount)
    crowded, usual = shares(amount, rows * top, limit, lean, True), shares(amount, rows * top, limit, lean, False)
    places = jnp.arange(amount)

    def named(tallies, rotation):
        used = int((tallies > 0).sum())
        fixed = max(1, used // 4)
        moved = fixed + (places - fixed + rotation * (used - fixed)) % max(1, amount - fixed)
        return jnp.zeros((amount,), jnp.int32).at[order[jnp.where(places < fixed, places, moved)]].set(jnp.asarray(tallies, jnp.int32))

    tallies = jnp.where(number % 4 == 0, named(crowded, number // 4), named(usual, number - number // 4 - 1))
    mixed = jax.random.permutation(jax.random.fold_in(own, 3), amount)
    giver, sink = mixed[0:amount // 2 * 2:2], mixed[1:amount // 2 * 2:2]
    room = jnp.minimum(tallies[giver] - 1, limit - tallies[sink]) // 2
    room = jnp.where((giver == order[0]) | (sink == order[0]) | (tallies[sink] == 0), 0, jnp.maximum(room, 0))
    moved = jax.random.randint(jax.random.fold_in(own, 4), (amount // 2,), 0, 1 << 20) % (room + 1)
    tallies = tallies.at[giver].add(-moved).at[sink].add(moved)
    items = jnp.searchsorted(jnp.cumsum(tallies), jnp.arange(rows * top), side="right").astype(jnp.int32)
    table = items.reshape(top, rows).T
    table = table[jax.random.permutation(jax.random.fold_in(own, 1), rows)]
    rotation = jax.random.randint(jax.random.fold_in(own, 2), (rows, 1), 0, top)
    return jnp.take_along_axis(table, (jnp.arange(top)[None, :] + rotation) % top, axis=1)


def shares(amount, total, bound, skew, full):
    weights = [(1 << 20) // math.isqrt(grade ** skew) + 1 for grade in range(1, amount + 1)]
    largest = bound if full else min(bound, max(-(-total // amount), total * weights[0] // sum(weights)))
    least = 1 if total - largest >= amount - 1 else 0
    counts, surplus = [largest] + [least] * (amount - 1), total - largest - least * (amount - 1)
    while surplus > 0:
        free = [i for i in range(1, amount) if counts[i] < largest] or [i for i in range(1, amount) if counts[i] < bound]
        mass, remaining = sum([weights[i] for i in free]), surplus
        for i in free:
            more = min(bound - counts[i], max(1, remaining * weights[i] // mass), surplus)
            counts[i] = counts[i] + more
            surplus = surplus - more
    return np.array(counts)


def scatter_about(own_key, dims, scale, bound, shards=(), held_as=jnp.bfloat16):
    array = jax.random.normal(own_key, dims, jnp.float32) * scale
    if len(shards) > 0:
        array = block_levels(own_key, dims, shards, -0.22, 0.18) * array
    return jnp.clip(array, min=-bound, max=bound).astype(held_as)


def setup_inputs(seed: int = 0) -> dict:
    keys = jax.random.split(jax.random.key(seed), 13)
    queries = draw_queries(jax.random.fold_in(keys[12], 71), 0)
    key_vectors = draw_key_vectors(jax.random.fold_in(keys[12], 71), 0)
    value_vectors = scatter_about(keys[2], (TOKEN_POSITIONS, HEAD_COUNT * HEAD_DIM), 1.5, 9.0, ((0, 16), (1, 16)))
    cumulative_gate = draw_cumulative_gate(jax.random.fold_in(keys[12], 71), 0)
    out_weight = scatter_about(keys[4], (HEAD_COUNT * HEAD_DIM, D), (HEAD_COUNT * HEAD_DIM) ** -0.5, 0.1875, ((0, 16),))
    expert_tokens = scatter_about(keys[5], (EXP_TOKENS, D), 1.0, 6.0, ((0, 256),))
    norm_gain = jnp.clip(1.0 + 0.18 * jax.random.normal(keys[6], (D,), jnp.float32), 0.1, 1.9)
    gate_weight = scatter_about(keys[7], (EXPERTS, D, FF), (D // 9) ** -0.5, 0.375, ((0, 16), (2, 16)))
    up_weight = scatter_about(keys[8], (EXPERTS, D, FF), (D // 9) ** -0.5, 0.375, ((0, 16), (2, 16)))
    down_weight = scatter_about(keys[9], (EXPERTS, FF, D), (FF * 64) ** -0.5, 0.015625, ((0, 16), (1, 16)))
    expert_choice_keys = jax.random.split(jax.random.fold_in(keys[10], 1), EXP_TOKENS // TOK_DEV)
    expert_choice_turns = jax.random.permutation(jax.random.fold_in(keys[10], 3), EXP_TOKENS // TOK_DEV)
    expert_choice = jax.vmap(lambda own, number: deal_out(jax.random.fold_in(keys[10], 2), own, number, TOK_DEV, EXPERTS, TOPK, CAP, 1))(expert_choice_keys, expert_choice_turns).reshape((EXP_TOKENS, TOPK))
    route_weights = jnp.clip(0.2 + 0.8 * jax.random.uniform(keys[11], (EXP_TOKENS, TOPK), jnp.float32) ** block_levels(keys[11], (EXP_TOKENS, TOPK), ((0, 256),), -0.2, 0.2), 0.2, 1.0)
    return {"queries": queries, "key_vectors": key_vectors, "value_vectors": value_vectors, "cumulative_gate": cumulative_gate, "out_weight": out_weight, "expert_tokens": expert_tokens, "norm_gain": norm_gain, "gate_weight": gate_weight, "up_weight": up_weight, "down_weight": down_weight, "expert_choice": expert_choice, "route_weights": route_weights}


eps_norm = 1e-05
clamp_limit = 7.0
sig_alpha = 1.702

def mixer_part(queries, key_vectors, value_vectors, cumulative_gate, out_weight):
    total_rows = queries.shape[0]
    block_size = min(512, total_rows)
    block_count = total_rows // block_size
    score_scale = 1.0 / math.sqrt(HEAD_DIM)
    key_pos = jnp.arange(total_rows, dtype=jnp.int32)

    def single_head(head_index):
        first_column = (head_index * HEAD_DIM).astype(jnp.int32)
        head_queries = lax.dynamic_slice_in_dim(queries, first_column, HEAD_DIM, 1)
        head_keys = lax.dynamic_slice_in_dim(key_vectors, first_column, HEAD_DIM, 1)
        head_values = lax.dynamic_slice_in_dim(value_vectors, first_column, HEAD_DIM, 1)
        head_gates = lax.dynamic_slice_in_dim(cumulative_gate, head_index.astype(jnp.int32), 1, 1)[:, 0]

        def one_block(block_index):
            row_start = (block_index * block_size).astype(jnp.int32)
            block_queries = lax.dynamic_slice_in_dim(head_queries, row_start, block_size, 0)
            block_gates = lax.dynamic_slice_in_dim(head_gates, row_start, block_size, 0)
            scores = jnp.dot(block_queries, head_keys.T, preferred_element_type=jnp.float32) * score_scale
            scores = scores + block_gates[:, None] - head_gates[None, :]
            query_pos = row_start + jnp.arange(block_size, dtype=jnp.int32)
            causal = key_pos[None, :] <= query_pos[:, None]
            scores = jnp.where(causal, scores, -jnp.inf)
            row_peak = lax.optimization_barrier(jnp.max(scores, axis=1, keepdims=True))
            weights = jnp.where(causal, jnp.exp(scores - row_peak), 0.0)
            numer = jnp.dot(weights.astype(jnp.bfloat16), head_values, preferred_element_type=jnp.float32)
            return (numer / lax.optimization_barrier(jnp.sum(weights, axis=1, keepdims=True))).astype(jnp.bfloat16)
        return lax.map(one_block, jnp.arange(block_count, dtype=jnp.int32)).reshape(total_rows, HEAD_DIM)
    per_head = lax.map(single_head, jnp.arange(HEAD_COUNT, dtype=jnp.int32))
    attention = jnp.transpose(per_head, (1, 0, 2)).reshape(total_rows, HEAD_COUNT * HEAD_DIM)
    group_width = HEAD_COUNT // N_TP * HEAD_DIM

    def add_group(running_total, group_index):
        first_column = (group_index * group_width).astype(jnp.int32)
        columns = lax.dynamic_slice_in_dim(attention, first_column, group_width, 1)
        weight_rows = lax.dynamic_slice_in_dim(out_weight, first_column, group_width, 0)
        partial_sum = jnp.dot(columns, weight_rows, preferred_element_type=jnp.float32).astype(jnp.bfloat16)
        partial_sum = lax.optimization_barrier(partial_sum)
        return (running_total + partial_sum.astype(jnp.float32), None)
    summed, unused = lax.scan(add_group, jnp.zeros((total_rows, D), jnp.float32), jnp.arange(N_TP, dtype=jnp.int32))
    return summed.astype(jnp.bfloat16)

def expert_part(expert_tokens, norm_gain, gate_weight, up_weight, down_weight, expert_choice, route_weights):
    total_rows = expert_tokens.shape[0]
    block_count = total_rows // TOK_DEV
    tokens_float = expert_tokens.astype(jnp.float32)
    normed = (tokens_float * lax.rsqrt(lax.optimization_barrier(jnp.mean(tokens_float * tokens_float, axis=1, keepdims=True)) + eps_norm) * norm_gain).astype(jnp.bfloat16)
    flat_ids = expert_choice.reshape(block_count, TOK_DEV * TOPK).astype(jnp.int32)
    one_hot = (flat_ids[:, :, None] == jnp.arange(EXPERTS, dtype=jnp.int32)[None, None, :]).astype(jnp.int32)
    slot_rank = lax.optimization_barrier(jnp.sum((jnp.cumsum(one_hot, axis=1) - one_hot) * one_hot, axis=2))
    block_ids = jnp.arange(block_count, dtype=jnp.int32)[:, None]
    destination = (flat_ids * (block_count * CAP) + block_ids * CAP + slot_rank).reshape(-1)
    token_ids = (block_ids * TOK_DEV + jnp.arange(TOK_DEV * TOPK, dtype=jnp.int32)[None, :] // TOPK).reshape(-1)
    slot_rows = jnp.zeros((EXPERTS * block_count * CAP, D), jnp.bfloat16).at[destination].set(normed[token_ids])
    slot_rows = slot_rows.reshape(EXPERTS, block_count * CAP, D)
    unit_group = FF // N_TP

    def single_expert(operands):
        rows_in, gate_matrix, up_matrix, down_matrix = operands
        gate_pre = jnp.minimum(jnp.dot(rows_in, gate_matrix, preferred_element_type=jnp.float32), clamp_limit)
        up_pre = jnp.clip(jnp.dot(rows_in, up_matrix, preferred_element_type=jnp.float32), -clamp_limit, clamp_limit)
        activation = (gate_pre * jax.nn.sigmoid(sig_alpha * gate_pre) * (up_pre + 1.0)).astype(jnp.bfloat16)

        def add_group(running_total, group_index):
            first_unit = (group_index * unit_group).astype(jnp.int32)
            columns = lax.dynamic_slice_in_dim(activation, first_unit, unit_group, 1)
            weight_rows = lax.dynamic_slice_in_dim(down_matrix, first_unit, unit_group, 0)
            partial_sum = jnp.dot(columns, weight_rows, preferred_element_type=jnp.float32).astype(jnp.bfloat16)
            partial_sum = lax.optimization_barrier(partial_sum)
            return (running_total + partial_sum.astype(jnp.float32), None)
        summed, unused = lax.scan(add_group, jnp.zeros((rows_in.shape[0], D), jnp.float32), jnp.arange(N_TP, dtype=jnp.int32))
        return summed.astype(jnp.bfloat16)
    results = lax.map(single_expert, (slot_rows, gate_weight, up_weight, down_weight)).reshape(EXPERTS * block_count * CAP, D)
    picked = results[destination].astype(jnp.float32).reshape(total_rows, TOPK, D)
    return lax.optimization_barrier(jnp.sum(picked * route_weights[:, :, None], axis=1)).astype(jnp.bfloat16)

def reference(queries, key_vectors, value_vectors, cumulative_gate, out_weight, expert_tokens, norm_gain, gate_weight, up_weight, down_weight, expert_choice, route_weights):
    mixer_output = mixer_part(queries, key_vectors, value_vectors, cumulative_gate, out_weight)
    expert_output = expert_part(expert_tokens, norm_gain, gate_weight, up_weight, down_weight, expert_choice, route_weights)
    return (mixer_output, expert_output)
```

```python
import jax
import jax.numpy as jnp
from jax import lax
from jax.experimental import pallas as pl
from jax.experimental.pallas import tpu as pltpu
from jax.sharding import PartitionSpec as P

EXPERTS = 16
PAD = 16
BLOCK = 1024
HEAD = 64
EPS = 1e-05
CLAMP = 7.0
ALPHA = 1.702
TILE = 256
NEG = float("-inf")
F32 = jnp.float32
BF16 = jnp.bfloat16


def whole(shape):
    return pl.BlockSpec(shape, lambda *_: (0,) * len(shape))


def params(limit=16 << 20):
    return pltpu.CompilerParams(vmem_limit_bytes=limit)


def slots_of(choice):
    rows = choice.shape[0]
    first, second = choice[:, 0:1], choice[:, 1:2]
    lane = lax.broadcasted_iota(jnp.int32, (rows, 128), 1)
    pick0 = (lane == first).astype(F32)
    pick1 = (lane == second).astype(F32)
    below = (
        lax.broadcasted_iota(jnp.int32, (rows, rows), 1)
        < lax.broadcasted_iota(jnp.int32, (rows, rows), 0)
    ).astype(F32)
    before = jnp.dot(
        below.astype(BF16), (pick0 + pick1).astype(BF16), preferred_element_type=F32
    )
    rank0 = jnp.sum(before * pick0, axis=1, keepdims=True).astype(jnp.int32)
    rank1 = jnp.sum(before * pick1, axis=1, keepdims=True).astype(jnp.int32)
    return first * PAD + rank0, second * PAD + rank1


def dispatch_body(tokens_ref, gain_ref, choice_ref, out_ref):
    x = tokens_ref[...].astype(F32)
    scale = lax.rsqrt(jnp.mean(x * x, axis=1, keepdims=True) + EPS)
    normed = (x * scale * gain_ref[...]).astype(BF16)
    slot0, slot1 = slots_of(choice_ref[...])
    lane = lax.broadcasted_iota(jnp.int32, (x.shape[0], EXPERTS * PAD), 1)
    placing = jnp.where((lane == slot0) | (lane == slot1), 1.0, 0.0).astype(BF16)
    out_ref[...] = lax.dot_general(
        placing, normed, (((0,), (0,)), ((), ())), preferred_element_type=F32
    ).astype(BF16)


def dispatch(tokens, gain, choice):
    return pl.pallas_call(
        dispatch_body,
        out_shape=jax.ShapeDtypeStruct((EXPERTS * PAD, tokens.shape[1]), BF16),
        compiler_params=params(),
        name="dispatch",
    )(tokens, gain, choice)


def combine_body(own_ref, choice_ref, weight_ref, out_ref):
    slot0, slot1 = slots_of(choice_ref[...])
    w = weight_ref[...]
    lane = lax.broadcasted_iota(jnp.int32, (w.shape[0], EXPERTS * PAD), 1)
    mix = jnp.where(lane == slot0, w[:, 0:1], 0.0) + jnp.where(lane == slot1, w[:, 1:2], 0.0)
    high = mix.astype(BF16)
    low = (mix - high.astype(F32)).astype(BF16)
    rows = own_ref[...]
    out_ref[...] = (
        jnp.dot(high, rows, preferred_element_type=F32)
        + jnp.dot(low, rows, preferred_element_type=F32)
    ).astype(BF16)


def combine(returned, choice, weights):
    return pl.pallas_call(
        combine_body,
        out_shape=jax.ShapeDtypeStruct((choice.shape[0], returned.shape[1]), BF16),
        compiler_params=params(),
        name="combine",
    )(returned, choice, weights)


def gated(gate_pre, up_pre):
    g = jnp.minimum(gate_pre, CLAMP)
    u = jnp.clip(up_pre, -CLAMP, CLAMP)
    return (g * jax.nn.sigmoid(ALPHA * g) * (u + 1.0)).astype(BF16)


def nt(a, b):
    return lax.dot_general(a, b, (((1,), (1,)), ((), ())), preferred_element_type=F32)


def hidden(rows, gu_refs):
    acts = []
    for gu in gu_refs:
        pre = jnp.dot(
            rows, jnp.concatenate([gu[0], gu[1]], axis=1), preferred_element_type=F32
        )
        acts.append(gated(pre[:, :128], pre[:, 128:]))
    return jnp.concatenate(acts, axis=1) if len(acts) > 1 else acts[0]


def stacked(d_refs):
    downs = [d[...] for d in d_refs]
    return jnp.concatenate(downs, axis=0) if len(downs) > 1 else downs[0]


def experts(x, gus, downs, y, first=0, count=None, keep=True):
    d = x.shape[1]
    n = len(gus)
    count = x.shape[0] // 256 if count is None else count

    def body(*refs):
        x_ref, gu_refs, d_refs, out_ref = refs[0], refs[1 : 1 + n], refs[1 + n : 1 + 2 * n], refs[-1]
        total = jnp.dot(
            hidden(x_ref[...], gu_refs), stacked(d_refs), preferred_element_type=F32
        )
        if y is not None:
            total = total + refs[-2][...].astype(F32)
        out_ref[...] = total.astype(BF16)

    rows = pl.BlockSpec((256, d), lambda i: (i + first, 0))
    args = [x, *gus, *downs] + ([] if y is None else [y])
    specs = [rows] + [whole(w.shape) for w in (*gus, *downs)] + ([] if y is None else [rows])
    return pl.pallas_call(
        body,
        grid=(count,),
        in_specs=specs,
        out_specs=pl.BlockSpec((256, d), lambda i: (i, 0)),
        out_shape=pltpu.HBM((count * 256, d), BF16) if keep else jax.ShapeDtypeStruct((count * 256, d), BF16),
        compiler_params=params(),
        name="experts",
        cost_estimate=pl.CostEstimate(
            flops=6 * count * 256 * d * 128 * n,
            transcendentals=count * 256 * 128,
            bytes_accessed=6 << 20,
        ),
    )(*args)


def attend(ep, base, q, kvg, state, first, last, finish):
    tiles = BLOCK // TILE

    def body(ep_ref, base_ref, q_ref, kv_ref, *rest):
        if state is not None:
            m_in, acc_in = rest[0], rest[1]
            rest = rest[2:]
        if finish:
            out_ref, m_ref, acc_ref = rest
        else:
            m_ref, acc_ref = rest
        if state is None:
            m_ref[...] = jnp.full(m_ref.shape, NEG, F32)
            acc_ref[...] = jnp.zeros(acc_ref.shape, F32)
        else:
            m_ref[...] = m_in[...]
            acc_ref[...] = acc_in[...]
        me = ep_ref[0]
        base = base_ref[...]
        lane = lax.broadcasted_iota(jnp.int32, (BLOCK, 128), 1)

        def one(j, masked):
            kv = kv_ref[j, 0:BLOCK, :]
            parts = kv_ref[j, BLOCK : BLOCK + 32, :].astype(F32)
            gates = (parts[0:8] + parts[8:16]) + parts[16:24]
            decay = base - gates
            row = jnp.concatenate([decay[c : c + 1] for c in range(8)], axis=1)
            values = jnp.where(lane < HEAD, jnp.ones_like(kv), kv)

            def scores(t):
                return nt(q_ref[t * TILE : (t + 1) * TILE, :], kv)

            ahead = scores(0)
            for t in range(tiles):
                s = ahead
                if t + 1 < tiles:
                    ahead = scores(t + 1)
                at = slice(t * TILE, (t + 1) * TILE)
                s = s + row
                if masked:
                    qpos = t * TILE + lax.broadcasted_iota(jnp.int32, (TILE, BLOCK), 0)
                    kpos = lax.broadcasted_iota(jnp.int32, (TILE, BLOCK), 1)
                    s = jnp.where(kpos <= qpos, s, NEG)
                old = m_ref[at, :]
                peak = jnp.maximum(
                    old, jnp.broadcast_to(jnp.max(s, axis=1, keepdims=True), (TILE, 128))
                )
                weight = jnp.exp(s - jnp.concatenate([peak] * (BLOCK // 128), axis=1))
                acc_ref[at, :] = acc_ref[at, :] * jnp.exp(old - peak) + jnp.dot(
                    weight.astype(BF16), values, preferred_element_type=F32
                )
                m_ref[at, :] = peak

        def step(j, carry):
            one(j - first, False)
            return carry

        lax.fori_loop(first, jnp.minimum(me, last), step, 0)

        @pl.when((me >= first) & (me < last))
        def _():
            one(me - first, True)

        if finish:
            for g in range(BLOCK // 64):
                a = acc_ref[64 * g : 64 * g + 32, :]
                b = acc_ref[64 * g + 32 : 64 * g + 64, :]
                pair = [a[:, HEAD:] / a[:, :HEAD], b[:, HEAD:] / b[:, :HEAD]]
                out_ref[32 * g : 32 * g + 32, :] = jnp.concatenate(pair, axis=1).astype(BF16)

    span = last - first
    args = [ep, base, q, kvg]
    specs = [
        pl.BlockSpec(memory_space=pltpu.SMEM),
        whole(base.shape),
        whole(q.shape),
        pl.BlockSpec((span,) + kvg.shape[1:], lambda *_: (first // span, 0, 0)),
    ]
    wide = jax.ShapeDtypeStruct((BLOCK, 128), F32)
    if state is not None:
        args += list(state)
        specs += [whole(wide.shape)] * 2
    if finish:
        outs = jax.ShapeDtypeStruct((BLOCK // 2, 2 * HEAD), BF16)
        out_specs = whole(outs.shape)
        scratch = [pltpu.VMEM(wide.shape, F32)] * 2
    else:
        outs = (wide, wide)
        out_specs = (whole(wide.shape),) * 2
        scratch = []
    return pl.pallas_call(
        body,
        grid=(1,),
        in_specs=specs,
        out_specs=out_specs,
        out_shape=outs,
        scratch_shapes=scratch,
        compiler_params=params(),
        name="attend",
        cost_estimate=pl.CostEstimate(
            flops=span * BLOCK * BLOCK * 1024, transcendentals=0, bytes_accessed=4 << 20
        ),
    )(*args)


def arrange(place, near):
    n = len(near)

    def body(place_ref, *refs):
        out_ref = refs[-1]
        chip = lax.div(place_ref[0], 2)
        core = lax.rem(place_ref[0], 2)
        for s in range(n):
            at = lax.rem(chip + s, n) * 2 * HEAD
            mine = pl.multiple_of(at + core * HEAD, HEAD)
            other = pl.multiple_of(at + (1 - core) * HEAD, HEAD)
            out_ref[pl.ds(mine, HEAD), :] = refs[s][:HEAD, :]
            out_ref[pl.ds(other, HEAD), :] = refs[s][HEAD:, :]

    return pl.pallas_call(
        body,
        grid=(1,),
        in_specs=[pl.BlockSpec(memory_space=pltpu.SMEM)] + [whole(a.shape) for a in near],
        out_specs=whole((n * 2 * HEAD, 128)),
        out_shape=jax.ShapeDtypeStruct((n * 2 * HEAD, 128), BF16),
        compiler_params=params(),
        name="arrange",
    )(place, *near)


def project(packed, columns):
    heads, half, _ = packed.shape
    width = heads * HEAD

    def body(a_ref, w_ref, out_ref, rows_ref):
        @pl.when(pl.program_id(0) == 0)
        def _():
            for h in range(0, heads, 2):
                a, b = a_ref[h].astype(F32), a_ref[h + 1].astype(F32)
                at = slice(h * HEAD, (h + 2) * HEAD)
                top = jnp.concatenate([a[:, :HEAD], b[:, :HEAD]], axis=1)
                low = jnp.concatenate([a[:, HEAD:], b[:, HEAD:]], axis=1)
                rows_ref[:half, at] = top.astype(BF16)
                rows_ref[half:, at] = low.astype(BF16)

        both = jnp.concatenate([w_ref[0], w_ref[1]], axis=1)
        out_ref[...] = jnp.dot(rows_ref[...], both, preferred_element_type=F32).astype(BF16)

    return pl.pallas_call(
        body,
        grid=(columns.shape[0] // 2,),
        in_specs=[whole(packed.shape), pl.BlockSpec((2, width, 128), lambda i: (i, 0, 0))],
        out_specs=pl.BlockSpec((2 * half, 256), lambda i: (0, i)),
        out_shape=jax.ShapeDtypeStruct((2 * half, columns.shape[0] * 128), BF16),
        scratch_shapes=[pltpu.VMEM((2 * half, width), BF16)],
        compiler_params=params(),
        name="project",
    )(packed, columns)


def local(
    queries,
    key_vectors,
    value_vectors,
    cumulative_gate,
    out_weight,
    expert_tokens,
    norm_gain,
    gate_weight,
    up_weight,
    down_weight,
    expert_choice,
    route_weights,
):
    n_tp = lax.axis_size("tp")
    n_ep = lax.axis_size("ep")
    chips = n_tp // 2
    d = expert_tokens.shape[1]
    spot = [(z, c) for z in range(chips) for c in range(2)]
    ahead = [(2 * z + c, 2 * ((z + 1 - 2 * c) % chips) + c) for z, c in spot]
    back = [(2 * z + c, 2 * ((z - 1 + 2 * c) % chips) + c) for z, c in spot]
    swap = [(2 * z + c, 2 * z + 1 - c) for z, c in spot]
    fence = lax.optimization_barrier

    def ring(a, b):
        return lax.ppermute(a, "tp", ahead), lax.ppermute(b, "tp", back)

    down = down_weight[0]
    da1, db1 = ring(down, down)
    gu = jnp.concatenate([gate_weight, up_weight], axis=0)
    ga1, gb1 = ring(gu, gu)

    high = lax.reduce_precision(cumulative_gate, 8, 7)
    mid = lax.reduce_precision(cumulative_gate - high, 8, 7)
    low = cumulative_gate - high - mid
    gates = jnp.concatenate([high, mid, low, jnp.zeros_like(low)], axis=1)
    gates = gates.T.reshape(32, 128).astype(BF16)
    packed = jnp.concatenate(
        [jnp.concatenate([key_vectors, value_vectors], axis=1), gates], axis=0
    )
    gain = norm_gain[None, :]
    outgoing = dispatch(expert_tokens, gain, expert_choice).reshape(n_ep, PAD, d)
    kvg = lax.all_gather(packed, "ep", axis=0)
    arrived = lax.all_to_all(outgoing, "ep", split_axis=0, concat_axis=0, tiled=True)
    ep = lax.axis_index("ep").astype(jnp.int32).reshape(1)
    q = jnp.concatenate([queries * BF16(0.125), jnp.zeros_like(queries)], axis=1)
    base = jnp.broadcast_to(cumulative_gate[0:1, :], (1, 128))
    strip = lax.dynamic_slice_in_dim(out_weight, lax.axis_index("ep") * 128, 128, 1)
    strip = jnp.concatenate([strip, lax.ppermute(strip, "tp", swap)], axis=0)
    da1, db1, strip = fence((da1, db1, strip))

    da2, db2 = ring(da1, db1)
    near = [strip] + [
        lax.ppermute(
            strip, "tp", [(2 * z + c, 2 * ((z - s) % chips) + c) for z, c in spot]
        )
        for s in range(1, chips)
    ]
    strips = arrange(lax.axis_index("tp").astype(jnp.int32).reshape(1), near)
    ga1, gb1, q, base = fence((ga1, gb1, q, base))

    ga2, gb2 = ring(ga1, gb1)
    columns = lax.all_gather(strips, "ep", axis=0)
    arrived = arrived.reshape(n_ep * PAD, d)
    beside = lax.ppermute(arrived, "tp", swap)
    x = jnp.concatenate([arrived, beside], axis=0)
    y = experts(x, [gu, ga1], [down, da1], None)
    da2, db2, y = fence((da2, db2, y))

    da3, db3 = ring(da2, db2)
    half = n_ep // 2
    y = experts(x, [gb1], [db1], y)
    state = attend(ep, base, q, kvg, None, 0, half, False)
    ga2, gb2, y, state = fence((ga2, gb2, y, state))

    ga3, gb3 = ring(ga2, gb2)
    attention = attend(ep, base, q, kvg, state, half, n_ep, True)
    da3, db3, attention = fence((da3, db3, attention))

    d4 = lax.ppermute(db3, "tp", back)
    y = experts(x, [ga2, gb2], [da2, db2], y)
    ga3, gb3, y, attention = fence((ga3, gb3, y, attention))
    rows = lax.all_to_all(
        attention.reshape(n_tp, -1, 2 * HEAD), "tp", split_axis=0, concat_axis=0, tiled=True
    )

    g4 = lax.ppermute(ga3, "tp", ahead)
    y = experts(x, [ga3, gb3], [da3, db3], y)
    g4, d4, y, rows = fence((g4, d4, y, rows))

    theirs = experts(x, [g4], [d4], y, 1, 1, False)
    extra = lax.ppermute(theirs, "tp", swap)
    mine = experts(x, [g4], [d4], y, 0, 1, False)
    results = (mine.astype(F32) + extra.astype(F32)).astype(BF16).reshape(n_ep, PAD, d)
    returned = lax.all_to_all(results, "ep", split_axis=0, concat_axis=0, tiled=True)
    rows, results = fence((rows, results))
    mixer_output = project(rows, columns)
    expert_output = combine(returned.reshape(n_ep * PAD, d), expert_choice, route_weights)
    return (mixer_output, expert_output)


def solution(mesh):
    placed = (
        P("ep", "tp"),
        P("ep", "tp"),
        P("ep", "tp"),
        P("ep", "tp"),
        P("tp", None),
        P(("ep", "tp"), None),
        P(),
        P("ep", None, "tp"),
        P("ep", None, "tp"),
        P("ep", "tp", None),
        P(("ep", "tp"), None),
        P(("ep", "tp"), None),
    )

    return jax.shard_map(
        local,
        mesh=mesh,
        in_specs=placed,
        out_specs=(P(("ep", "tp"), None), P(("ep", "tp"), None)),
        check_vma=False,
    )
```

```python
import jax
import jax.numpy as jnp
from jax import lax
from jax.experimental import pallas as pl
from jax.experimental.pallas import tpu as pltpu
from jax.sharding import PartitionSpec as P

EXPERTS = 16
PAD = 16
BLOCK = 1024
HEAD = 64
EPS = 1e-05
CLAMP = 7.0
ALPHA = 1.702
TILE = 256
NEG = float("-inf")
F32 = jnp.float32
BF16 = jnp.bfloat16


def whole(shape):
    return pl.BlockSpec(shape, lambda *_: (0,) * len(shape))


def held(*arrays):
    return [pltpu.with_memory_space_constraint(a, pltpu.HBM) for a in arrays]


def params(limit=16 << 20):
    return pltpu.CompilerParams(vmem_limit_bytes=limit)


def slots_of(choice):
    rows = choice.shape[0]
    first, second = choice[:, 0:1], choice[:, 1:2]
    lane = lax.broadcasted_iota(jnp.int32, (rows, 128), 1)
    pick0 = (lane == first).astype(F32)
    pick1 = (lane == second).astype(F32)
    below = (
        lax.broadcasted_iota(jnp.int32, (rows, rows), 1)
        < lax.broadcasted_iota(jnp.int32, (rows, rows), 0)
    ).astype(F32)
    before = jnp.dot(
        below.astype(BF16), (pick0 + pick1).astype(BF16), preferred_element_type=F32
    )
    rank0 = jnp.sum(before * pick0, axis=1, keepdims=True).astype(jnp.int32)
    rank1 = jnp.sum(before * pick1, axis=1, keepdims=True).astype(jnp.int32)
    return first * PAD + rank0, second * PAD + rank1


def dispatch_body(tokens_ref, gain_ref, choice_ref, out_ref):
    x = tokens_ref[...].astype(F32)
    scale = lax.rsqrt(jnp.mean(x * x, axis=1, keepdims=True) + EPS)
    normed = (x * scale * gain_ref[...]).astype(BF16)
    slot0, slot1 = slots_of(choice_ref[...])
    lane = lax.broadcasted_iota(jnp.int32, (x.shape[0], EXPERTS * PAD), 1)
    placing = jnp.where((lane == slot0) | (lane == slot1), 1.0, 0.0).astype(BF16)
    out_ref[...] = lax.dot_general(
        placing, normed, (((0,), (0,)), ((), ())), preferred_element_type=F32
    ).astype(BF16)


def dispatch(tokens, gain, choice):
    return pl.pallas_call(
        dispatch_body,
        out_shape=jax.ShapeDtypeStruct((EXPERTS * PAD, tokens.shape[1]), BF16),
        compiler_params=params(),
        name="dispatch",
    )(tokens, gain, choice)


def combine_body(own_ref, choice_ref, weight_ref, out_ref):
    slot0, slot1 = slots_of(choice_ref[...])
    w = weight_ref[...]
    lane = lax.broadcasted_iota(jnp.int32, (w.shape[0], EXPERTS * PAD), 1)
    mix = jnp.where(lane == slot0, w[:, 0:1], 0.0) + jnp.where(lane == slot1, w[:, 1:2], 0.0)
    high = mix.astype(BF16)
    low = (mix - high.astype(F32)).astype(BF16)
    rows = own_ref[...]
    out_ref[...] = (
        jnp.dot(high, rows, preferred_element_type=F32)
        + jnp.dot(low, rows, preferred_element_type=F32)
    ).astype(BF16)


def combine(returned, choice, weights):
    return pl.pallas_call(
        combine_body,
        out_shape=jax.ShapeDtypeStruct((choice.shape[0], returned.shape[1]), BF16),
        compiler_params=params(),
        name="combine",
    )(returned, choice, weights)


def gated(gate_pre, up_pre):
    g = jnp.minimum(gate_pre, CLAMP)
    u = jnp.clip(up_pre, -CLAMP, CLAMP)
    return (g * jax.nn.sigmoid(ALPHA * g) * (u + 1.0)).astype(BF16)


def nt(a, b):
    return lax.dot_general(a, b, (((1,), (1,)), ((), ())), preferred_element_type=F32)


def experts(rows, gus, downs, y, first=0):
    n, m = len(gus), len(rows)
    count, d = sum(r.shape[0] for r in rows), rows[0].shape[1]
    each, wide = count // m, 512
    has_y = y is not None

    def body(*refs):
        row_refs, refs = refs[:m], refs[m:]
        gu_refs, refs = refs[:n], refs[n:]
        d_refs, refs = refs[:n], refs[n:]
        if has_y:
            y_ref, refs = refs[0], refs[1:]
        out_ref, x, gu, down, acts, old, new, sems, out_sems = refs
        x_in = [
            pltpu.make_async_copy(row_refs[k], x.at[pl.ds(k * each, each), :], sems.at[k])
            for k in range(m)
        ]
        gu_in = [pltpu.make_async_copy(gu_refs[c], gu.at[c], sems.at[m + c]) for c in range(n)]
        d_in = [
            pltpu.make_async_copy(
                d_refs[c], down.at[pl.ds(c * 128, 128), :], sems.at[m + n + c]
            )
            for c in range(n)
        ]
        for copy in x_in + gu_in + d_in:
            copy.start()
        if has_y:
            y_in = pltpu.make_async_copy(
                y_ref.at[pl.ds(first, count), :], old, sems.at[m + 2 * n]
            )
            y_in.start()
        for copy in x_in:
            copy.wait()

        def slice_of_hidden(c, carry):
            pltpu.make_async_copy(gu_refs[0], gu.at[c], sems.at[m + c]).wait()
            pre = jnp.dot(
                x[...], jnp.concatenate([gu[c, 0], gu[c, 1]], axis=1), preferred_element_type=F32
            )
            at = pl.multiple_of(c * 128, 128)
            acts[:, pl.ds(at, 128)] = gated(pre[:, :128], pre[:, 128:])
            return carry

        lax.fori_loop(0, n, slice_of_hidden, 0)
        for copy in d_in:
            copy.wait()
        if has_y:
            y_in.wait()

        def out_copy(t):
            to = pl.ds(pl.multiple_of(t * wide, wide), wide)
            return pltpu.make_async_copy(new.at[:, to], out_ref.at[:, to], out_sems.at[t])

        def slice_of_out(t, carry):
            at = pl.ds(pl.multiple_of(t * wide, wide), wide)
            total = jnp.dot(acts[...], down[:, at], preferred_element_type=F32)
            if has_y:
                total = total + old[:, at].astype(F32)
            new[:, at] = total.astype(BF16)
            out_copy(t).start()
            return carry

        lax.fori_loop(0, d // wide, slice_of_out, 0)
        for t in range(d // wide):
            out_copy(t).wait()

    args = held(*rows, *gus, *downs, *([y] if has_y else []))
    hbm = pl.BlockSpec(memory_space=pltpu.HBM)
    return pl.pallas_call(
        body,
        in_specs=[hbm] * len(args),
        out_specs=hbm,
        out_shape=pltpu.HBM((count, d), BF16),
        scratch_shapes=[
            pltpu.VMEM((count, d), BF16),
            pltpu.VMEM((n, 2, d, 128), BF16),
            pltpu.VMEM((n * 128, d), BF16),
            pltpu.VMEM((count, n * 128), BF16),
            pltpu.VMEM((count, d) if has_y else (16, 128), BF16),
            pltpu.VMEM((count, d), BF16),
            pltpu.SemaphoreType.DMA((m + 2 * n + 1,)),
            pltpu.SemaphoreType.DMA((d // wide,)),
        ],
        compiler_params=params(24 << 20),
        name="experts",
        cost_estimate=pl.CostEstimate(
            flops=6 * count * d * 128 * n,
            transcendentals=count * 128 * n,
            bytes_accessed=6 << 20,
        ),
    )(*args)


def experts_last(rows, gu, down, y, first):
    count, d = rows.shape

    def body(x_ref, gu_ref, d_ref, y_ref, out_ref):
        both = jnp.concatenate([gu_ref[0], gu_ref[1]], axis=1)
        pre = jnp.dot(x_ref[...], both, preferred_element_type=F32)
        total = jnp.dot(
            gated(pre[:, :128], pre[:, 128:]), d_ref[...], preferred_element_type=F32
        )
        out_ref[...] = (total + y_ref[...].astype(F32)).astype(BF16)

    x, old = held(rows, y)
    return pl.pallas_call(
        body,
        grid=(1,),
        in_specs=[
            whole((count, d)),
            whole(gu.shape),
            whole(down.shape),
            pl.BlockSpec((count, d), lambda i: (first // count, 0)),
        ],
        out_specs=whole((count, d)),
        out_shape=jax.ShapeDtypeStruct((count, d), BF16),
        compiler_params=params(),
        name="experts_last",
        cost_estimate=pl.CostEstimate(
            flops=6 * count * d * 128, transcendentals=count * 128, bytes_accessed=5 << 20
        ),
    )(x, gu, down, old)


def widen(queries):
    def body(q_ref, out_ref):
        scaled = (q_ref[...].astype(F32) * 0.125).astype(BF16)
        out_ref[...] = jnp.concatenate([scaled, jnp.zeros_like(scaled)], axis=1)

    return pl.pallas_call(
        body,
        out_shape=jax.ShapeDtypeStruct((queries.shape[0], 2 * queries.shape[1]), BF16),
        compiler_params=params(),
        name="widen",
    )(queries)


def attend(ep, base, q, kvg, state, first, last, finish):
    tiles = BLOCK // TILE

    def body(ep_ref, base_ref, q_ref, kvg_ref, *rest):
        kv_ref, sems = rest[-2:]
        rest = rest[:-2]

        def fetch(j):
            return pltpu.make_async_copy(kvg_ref.at[first + j], kv_ref.at[j], sems.at[j])

        for j in range(last - first):
            fetch(j).start()
        if state is not None:
            m_in, acc_in = rest[0], rest[1]
            rest = rest[2:]
        if finish:
            out_ref, m_ref, acc_ref = rest
        else:
            m_ref, acc_ref = rest
        if state is None:
            m_ref[...] = jnp.full(m_ref.shape, NEG, F32)
            acc_ref[...] = jnp.zeros(acc_ref.shape, F32)
        else:
            m_ref[...] = m_in[...]
            acc_ref[...] = acc_in[...]
        me = ep_ref[0]
        base = base_ref[...]
        lane = lax.broadcasted_iota(jnp.int32, (BLOCK, 128), 1)

        def one(j, masked):
            fetch(j).wait()
            kv = kv_ref[j, 0:BLOCK, :]
            parts = kv_ref[j, BLOCK : BLOCK + 32, :].astype(F32)
            gates = (parts[0:8] + parts[8:16]) + parts[16:24]
            decay = base - gates
            row = jnp.concatenate([decay[c : c + 1] for c in range(8)], axis=1)
            values = jnp.where(lane < HEAD, jnp.ones_like(kv), kv)

            def scores(t):
                return nt(q_ref[t * TILE : (t + 1) * TILE, :], kv)

            def update(t, s):
                at = slice(t * TILE, (t + 1) * TILE)
                s = s + row
                if masked:
                    qpos = t * TILE + lax.broadcasted_iota(jnp.int32, (TILE, BLOCK), 0)
                    kpos = lax.broadcasted_iota(jnp.int32, (TILE, BLOCK), 1)
                    s = jnp.where(kpos <= qpos, s, NEG)
                old = m_ref[at, :]
                peak = jnp.maximum(
                    old, jnp.broadcast_to(jnp.max(s, axis=1, keepdims=True), (TILE, 128))
                )
                weight = jnp.exp(s - jnp.concatenate([peak] * (BLOCK // 128), axis=1))
                acc_ref[at, :] = acc_ref[at, :] * jnp.exp(old - peak) + jnp.dot(
                    weight.astype(BF16), values, preferred_element_type=F32
                )
                m_ref[at, :] = peak

            ahead = scores(0)
            for t in range(tiles):
                s = ahead
                if t + 1 < tiles:
                    ahead = scores(t + 1)
                update(t, s)

        def step(j, carry):
            one(j - first, False)
            return carry

        lax.fori_loop(first, jnp.minimum(me, last), step, 0)

        @pl.when((me >= first) & (me < last))
        def _():
            one(me - first, True)

        def drop(j, carry):
            fetch(j - first).wait()
            return carry

        lax.fori_loop(jnp.maximum(jnp.minimum(me + 1, last), first), last, drop, 0)

        if finish:
            for g in range(BLOCK // 64):
                a = acc_ref[64 * g : 64 * g + 32, :]
                b = acc_ref[64 * g + 32 : 64 * g + 64, :]
                pair = [a[:, HEAD:] / a[:, :HEAD], b[:, HEAD:] / b[:, :HEAD]]
                out_ref[32 * g : 32 * g + 32, :] = jnp.concatenate(pair, axis=1).astype(BF16)

    span = last - first
    args = [ep, base, q, *held(kvg)]
    specs = [
        pl.BlockSpec(memory_space=pltpu.SMEM),
        whole(base.shape),
        whole(q.shape),
        pl.BlockSpec(memory_space=pltpu.HBM),
    ]
    wide = jax.ShapeDtypeStruct((BLOCK, 128), F32)
    if state is not None:
        args += list(state)
        specs += [whole(wide.shape)] * 2
    if finish:
        outs = jax.ShapeDtypeStruct((BLOCK // 2, 2 * HEAD), BF16)
        out_specs = whole(outs.shape)
        scratch = [pltpu.VMEM(wide.shape, F32)] * 2
    else:
        outs = (wide, wide)
        out_specs = (whole(wide.shape),) * 2
        scratch = []
    return pl.pallas_call(
        body,
        grid=(1,),
        in_specs=specs,
        out_specs=out_specs,
        out_shape=outs,
        scratch_shapes=scratch
        + [pltpu.VMEM((span,) + kvg.shape[1:], BF16), pltpu.SemaphoreType.DMA((span,))],
        compiler_params=params(),
        name="attend",
        cost_estimate=pl.CostEstimate(
            flops=span * BLOCK * BLOCK * 1024, transcendentals=0, bytes_accessed=4 << 20
        ),
    )(*args)


def arrange(place, low, high, far):
    each = low.shape[0] // HEAD

    def body(place_ref, low_ref, high_ref, far_ref, out_ref):
        chip = lax.div(place_ref[0], 2)
        core = lax.rem(place_ref[0], 2)
        for k in range(2 * each):
            at = jnp.bitwise_xor(chip, k) * 2 * HEAD
            mine = pl.multiple_of(at + core * HEAD, HEAD)
            other = pl.multiple_of(at + (1 - core) * HEAD, HEAD)
            near = low_ref if k < each else high_ref
            piece = slice((k % each) * HEAD, (k % each + 1) * HEAD)
            out_ref[pl.ds(mine, HEAD), :] = near[piece, :]
            out_ref[pl.ds(other, HEAD), :] = far_ref[k * HEAD : (k + 1) * HEAD, :]

    return pl.pallas_call(
        body,
        grid=(1,),
        in_specs=[pl.BlockSpec(memory_space=pltpu.SMEM)]
        + [whole(a.shape) for a in (low, high, far)],
        out_specs=whole((2 * far.shape[0], 128)),
        out_shape=jax.ShapeDtypeStruct((2 * far.shape[0], 128), BF16),
        compiler_params=params(),
        name="arrange",
    )(place, low, high, far)


def project(packed, columns):
    heads, half, _ = packed.shape
    width = heads * HEAD

    def body(a_ref, w_ref, out_ref, rows_ref):
        @pl.when(pl.program_id(0) == 0)
        def _():
            for h in range(0, heads, 2):
                a, b = a_ref[h].astype(F32), a_ref[h + 1].astype(F32)
                at = slice(h * HEAD, (h + 2) * HEAD)
                top = jnp.concatenate([a[:, :HEAD], b[:, :HEAD]], axis=1)
                low = jnp.concatenate([a[:, HEAD:], b[:, HEAD:]], axis=1)
                rows_ref[:half, at] = top.astype(BF16)
                rows_ref[half:, at] = low.astype(BF16)

        both = jnp.concatenate([w_ref[0], w_ref[1]], axis=1)
        out_ref[...] = jnp.dot(rows_ref[...], both, preferred_element_type=F32).astype(BF16)

    return pl.pallas_call(
        body,
        grid=(columns.shape[0] // 2,),
        in_specs=[whole(packed.shape), pl.BlockSpec((2, width, 128), lambda i: (i, 0, 0))],
        out_specs=pl.BlockSpec((2 * half, 256), lambda i: (0, i)),
        out_shape=jax.ShapeDtypeStruct((2 * half, columns.shape[0] * 128), BF16),
        scratch_shapes=[pltpu.VMEM((2 * half, width), BF16)],
        compiler_params=params(),
        name="project",
    )(packed, columns)


def local(
    queries,
    key_vectors,
    value_vectors,
    cumulative_gate,
    out_weight,
    expert_tokens,
    norm_gain,
    gate_weight,
    up_weight,
    down_weight,
    expert_choice,
    route_weights,
):
    n_tp = lax.axis_size("tp")
    n_ep = lax.axis_size("ep")
    chips = n_tp // 2
    d = expert_tokens.shape[1]
    spot = [(z, c) for z in range(chips) for c in range(2)]
    ahead = [(2 * z + c, 2 * ((z + 1 - 2 * c) % chips) + c) for z, c in spot]
    back = [(2 * z + c, 2 * ((z - 1 + 2 * c) % chips) + c) for z, c in spot]
    swap = [(2 * z + c, 2 * z + 1 - c) for z, c in spot]
    fence = lax.optimization_barrier

    def ring(a, b):
        return lax.ppermute(a, "tp", ahead), lax.ppermute(b, "tp", back)

    def across(a, bit):
        return lax.ppermute(a, "tp", [(2 * z + c, 2 * (z ^ bit) + c) for z, c in spot])

    strip = lax.dynamic_slice_in_dim(out_weight, lax.axis_index("ep") * 128, 128, 1)
    strip = jnp.concatenate([strip, across(strip, 1)], axis=0)
    down = down_weight[0]
    da1, db1 = ring(down, down)
    high = lax.reduce_precision(cumulative_gate, 8, 7)
    mid = lax.reduce_precision(cumulative_gate - high, 8, 7)
    low = cumulative_gate - high - mid
    gates = jnp.concatenate([high, mid, low, jnp.zeros_like(low)], axis=1)
    gates = gates.T.reshape(32, 128).astype(BF16)
    packed = jnp.concatenate(
        [jnp.concatenate([key_vectors, value_vectors], axis=1), gates], axis=0
    )
    kvg = lax.all_gather(packed, "ep", axis=0)
    packed, gate_weight, strip = fence((packed, gate_weight, strip))
    strip = jnp.concatenate([strip, across(strip, 2)], axis=0)
    gu = jnp.concatenate([gate_weight, up_weight], axis=0)
    ga1, gb1 = ring(gu, gu)

    gain = norm_gain[None, :]
    outgoing = dispatch(expert_tokens, gain, expert_choice).reshape(n_ep, PAD, d)
    arrived = lax.all_to_all(outgoing, "ep", split_axis=0, concat_axis=0, tiled=True)
    ep = lax.axis_index("ep").astype(jnp.int32).reshape(1)
    strips_high = across(strip, 4)
    q = widen(queries)
    base = jnp.broadcast_to(cumulative_gate[0:1, :], (1, 128))
    da1, db1 = fence((da1, db1))

    da2, db2 = ring(da1, db1)
    ga1, gb1, q, base = fence((ga1, gb1, q, base))

    ga2, gb2 = ring(ga1, gb1)
    far = lax.ppermute(jnp.concatenate([strip, strips_high], axis=0), "tp", swap)
    place = lax.axis_index("tp").astype(jnp.int32).reshape(1)
    strips = arrange(place, strip, strips_high, far)
    columns = lax.all_gather(strips, "ep", axis=0)
    arrived = arrived.reshape(n_ep * PAD, d)
    beside = lax.ppermute(arrived, "tp", swap)
    x = [arrived, beside]
    da2, db2 = fence((da2, db2))

    da3, db3 = ring(da2, db2)
    half = n_ep // 2
    y = experts(x, [gu, ga1, gb1], [down, da1, db1], None)
    state = attend(ep, base, q, kvg, None, 0, half, False)
    ga2, gb2, state = fence((ga2, gb2, state))

    ga3, gb3 = ring(ga2, gb2)
    d4 = lax.ppermute(db3, "tp", back)
    attention = attend(ep, base, q, kvg, state, half, n_ep, True)
    rows = lax.all_to_all(
        attention.reshape(n_tp, -1, 2 * HEAD), "tp", split_axis=0, concat_axis=0, tiled=True
    )
    ga3, gb3, y, attention = fence((ga3, gb3, y, attention))

    g4 = lax.ppermute(ga3, "tp", ahead)
    y = experts(x, [ga2, gb2, ga3, gb3], [da2, db2, da3, db3], y)
    g4, d4, y, rows = fence((g4, d4, y, rows))

    theirs = experts_last(beside, g4, d4, y, arrived.shape[0])
    extra = lax.ppermute(theirs, "tp", swap)
    mine = experts_last(arrived, g4, d4, y, 0)
    results = (mine.astype(F32) + extra.astype(F32)).astype(BF16).reshape(n_ep, PAD, d)
    returned = lax.all_to_all(results, "ep", split_axis=0, concat_axis=0, tiled=True)
    rows, results = fence((rows, results))
    mixer_output = project(rows, columns)
    expert_output = combine(returned.reshape(n_ep * PAD, d), expert_choice, route_weights)
    return (mixer_output, expert_output)


def solution(mesh):
    placed = (
        P("ep", "tp"),
        P("ep", "tp"),
        P("ep", "tp"),
        P("ep", "tp"),
        P("tp", None),
        P(("ep", "tp"), None),
        P(),
        P("ep", None, "tp"),
        P("ep", None, "tp"),
        P("ep", "tp", None),
        P(("ep", "tp"), None),
        P(("ep", "tp"), None),
    )

    return jax.shard_map(
        local,
        mesh=mesh,
        in_specs=placed,
        out_specs=(P(("ep", "tp"), None), P(("ep", "tp"), None)),
        check_vma=False,
    )
```

```python
import jax
import jax.numpy as jnp
from jax import lax
from jax.experimental import pallas as pl
from jax.experimental.pallas import tpu as pltpu
from jax.sharding import PartitionSpec as P

EXPERTS = 16
PAD = 16
BLOCK = 1024
HEAD = 64
EPS = 1e-05
CLAMP = 7.0
ALPHA = 1.702
TILE = 256
NEG = float("-inf")
F32 = jnp.float32
BF16 = jnp.bfloat16


def whole(shape):
    return pl.BlockSpec(shape, lambda *_: (0,) * len(shape))


def held(*arrays):
    return [pltpu.with_memory_space_constraint(a, pltpu.HBM) for a in arrays]


def params(limit=16 << 20):
    return pltpu.CompilerParams(vmem_limit_bytes=limit)


def slots_of(choice):
    rows = choice.shape[0]
    first, second = choice[:, 0:1], choice[:, 1:2]
    lane = lax.broadcasted_iota(jnp.int32, (rows, 128), 1)
    pick0 = (lane == first).astype(F32)
    pick1 = (lane == second).astype(F32)
    below = (
        lax.broadcasted_iota(jnp.int32, (rows, rows), 1)
        < lax.broadcasted_iota(jnp.int32, (rows, rows), 0)
    ).astype(F32)
    before = jnp.dot(
        below.astype(BF16), (pick0 + pick1).astype(BF16), preferred_element_type=F32
    )
    rank0 = jnp.sum(before * pick0, axis=1, keepdims=True).astype(jnp.int32)
    rank1 = jnp.sum(before * pick1, axis=1, keepdims=True).astype(jnp.int32)
    return first * PAD + rank0, second * PAD + rank1


def dispatch_body(tokens_ref, gain_ref, choice_ref, out_ref):
    x = tokens_ref[...].astype(F32)
    scale = lax.rsqrt(jnp.mean(x * x, axis=1, keepdims=True) + EPS)
    normed = (x * scale * gain_ref[...]).astype(BF16)
    slot0, slot1 = slots_of(choice_ref[...])
    lane = lax.broadcasted_iota(jnp.int32, (x.shape[0], EXPERTS * PAD), 1)
    placing = jnp.where((lane == slot0) | (lane == slot1), 1.0, 0.0).astype(BF16)
    out_ref[...] = lax.dot_general(
        placing, normed, (((0,), (0,)), ((), ())), preferred_element_type=F32
    ).astype(BF16)


def dispatch(tokens, gain, choice):
    return pl.pallas_call(
        dispatch_body,
        out_shape=jax.ShapeDtypeStruct((EXPERTS * PAD, tokens.shape[1]), BF16),
        compiler_params=params(),
        name="dispatch",
    )(tokens, gain, choice)


def mix_body(choice_ref, weight_ref, high_ref, low_ref):
    slot0, slot1 = slots_of(choice_ref[...])
    w = weight_ref[...]
    lane = lax.broadcasted_iota(jnp.int32, (w.shape[0], EXPERTS * PAD), 1)
    mix = jnp.where(lane == slot0, w[:, 0:1], 0.0) + jnp.where(lane == slot1, w[:, 1:2], 0.0)
    high = mix.astype(BF16)
    high_ref[...] = high
    low_ref[...] = (mix - high.astype(F32)).astype(BF16)


def mixing(choice, weights):
    part = jax.ShapeDtypeStruct((choice.shape[0], EXPERTS * PAD), BF16)
    return pl.pallas_call(
        mix_body, out_shape=(part, part), compiler_params=params(), name="mixing"
    )(choice, weights)


def combine_body(rows_ref, high_ref, low_ref, out_ref):
    rows = rows_ref[...]
    out_ref[...] = (
        jnp.dot(high_ref[...], rows, preferred_element_type=F32)
        + jnp.dot(low_ref[...], rows, preferred_element_type=F32)
    ).astype(BF16)


def combine(returned, high, low):
    return pl.pallas_call(
        combine_body,
        out_shape=jax.ShapeDtypeStruct((high.shape[0], returned.shape[1]), BF16),
        compiler_params=params(),
        name="combine",
    )(returned, high, low)


def gated(gate_pre, up_pre):
    g = jnp.minimum(gate_pre, CLAMP)
    u = jnp.clip(up_pre, -CLAMP, CLAMP)
    return (g * jax.nn.sigmoid(ALPHA * g) * (u + 1.0)).astype(BF16)


def nt(a, b):
    return lax.dot_general(a, b, (((1,), (1,)), ((), ())), preferred_element_type=F32)


def experts(rows, gus, downs, y, first=0):
    n, m = len(gus), len(rows)
    count, d = sum(r.shape[0] for r in rows), rows[0].shape[1]
    each, wide = count // m, 512
    has_y = y is not None

    def body(*refs):
        row_refs, refs = refs[:m], refs[m:]
        gu_refs, refs = refs[:n], refs[n:]
        d_refs, refs = refs[:n], refs[n:]
        if has_y:
            y_ref, refs = refs[0], refs[1:]
        out_ref, x, gu, down, acts, old, new, sems, out_sems = refs
        x_in = [
            pltpu.make_async_copy(row_refs[k], x.at[pl.ds(k * each, each), :], sems.at[k])
            for k in range(m)
        ]
        gu_in = [pltpu.make_async_copy(gu_refs[c], gu.at[c], sems.at[m + c]) for c in range(n)]
        d_in = [
            pltpu.make_async_copy(
                d_refs[c], down.at[pl.ds(c * 128, 128), :], sems.at[m + n + c]
            )
            for c in range(n)
        ]
        for copy in x_in + gu_in + d_in:
            copy.start()
        if has_y:
            y_in = pltpu.make_async_copy(
                y_ref.at[pl.ds(first, count), :], old, sems.at[m + 2 * n]
            )
            y_in.start()
        for copy in x_in:
            copy.wait()

        def slice_of_hidden(c, carry):
            pltpu.make_async_copy(gu_refs[0], gu.at[c], sems.at[m + c]).wait()
            pre = jnp.dot(
                x[...], jnp.concatenate([gu[c, 0], gu[c, 1]], axis=1), preferred_element_type=F32
            )
            at = pl.multiple_of(c * 128, 128)
            acts[:, pl.ds(at, 128)] = gated(pre[:, :128], pre[:, 128:])
            return carry

        lax.fori_loop(0, n, slice_of_hidden, 0)
        for copy in d_in:
            copy.wait()
        if has_y:
            y_in.wait()

        def out_copy(t):
            to = pl.ds(pl.multiple_of(t * wide, wide), wide)
            return pltpu.make_async_copy(new.at[:, to], out_ref.at[:, to], out_sems.at[t])

        def slice_of_out(t, carry):
            at = pl.ds(pl.multiple_of(t * wide, wide), wide)
            total = jnp.dot(acts[...], down[:, at], preferred_element_type=F32)
            if has_y:
                total = total + old[:, at].astype(F32)
            new[:, at] = total.astype(BF16)
            out_copy(t).start()
            return carry

        lax.fori_loop(0, d // wide, slice_of_out, 0)
        for t in range(d // wide):
            out_copy(t).wait()

    args = held(*rows, *gus, *downs, *([y] if has_y else []))
    hbm = pl.BlockSpec(memory_space=pltpu.HBM)
    return pl.pallas_call(
        body,
        in_specs=[hbm] * len(args),
        out_specs=hbm,
        out_shape=pltpu.HBM((count, d), BF16),
        scratch_shapes=[
            pltpu.VMEM((count, d), BF16),
            pltpu.VMEM((n, 2, d, 128), BF16),
            pltpu.VMEM((n * 128, d), BF16),
            pltpu.VMEM((count, n * 128), BF16),
            pltpu.VMEM((count, d) if has_y else (16, 128), BF16),
            pltpu.VMEM((count, d), BF16),
            pltpu.SemaphoreType.DMA((m + 2 * n + 1,)),
            pltpu.SemaphoreType.DMA((d // wide,)),
        ],
        compiler_params=params(24 << 20),
        name="experts",
        cost_estimate=pl.CostEstimate(
            flops=6 * count * d * 128 * n,
            transcendentals=count * 128 * n,
            bytes_accessed=6 << 20,
        ),
    )(*args)


def experts_last(rows, gu, down, y, first):
    count, d = rows.shape

    def body(x_ref, gu_ref, d_ref, y_ref, out_ref):
        both = jnp.concatenate([gu_ref[0], gu_ref[1]], axis=1)
        pre = jnp.dot(x_ref[...], both, preferred_element_type=F32)
        total = jnp.dot(
            gated(pre[:, :128], pre[:, 128:]), d_ref[...], preferred_element_type=F32
        )
        out_ref[...] = (total + y_ref[...].astype(F32)).astype(BF16)

    x, old = held(rows, y)
    return pl.pallas_call(
        body,
        grid=(1,),
        in_specs=[
            whole((count, d)),
            whole(gu.shape),
            whole(down.shape),
            pl.BlockSpec((count, d), lambda i: (first // count, 0)),
        ],
        out_specs=whole((count, d)),
        out_shape=jax.ShapeDtypeStruct((count, d), BF16),
        compiler_params=params(),
        name="experts_last",
        cost_estimate=pl.CostEstimate(
            flops=6 * count * d * 128, transcendentals=count * 128, bytes_accessed=5 << 20
        ),
    )(x, gu, down, old)


def widen(queries):
    def body(q_ref, out_ref):
        scaled = (q_ref[...].astype(F32) * 0.125).astype(BF16)
        out_ref[...] = jnp.concatenate([scaled, jnp.zeros_like(scaled)], axis=1)

    return pl.pallas_call(
        body,
        out_shape=jax.ShapeDtypeStruct((queries.shape[0], 2 * queries.shape[1]), BF16),
        compiler_params=params(),
        name="widen",
    )(queries)


def attend(ep, base, q, kvg, state, first, last, finish):
    tiles = BLOCK // TILE

    def body(ep_ref, base_ref, q_ref, kvg_ref, *rest):
        kv_ref, sems = rest[-2:]
        rest = rest[:-2]

        def fetch(j):
            return pltpu.make_async_copy(kvg_ref.at[first + j], kv_ref.at[j], sems.at[j])

        for j in range(last - first):
            fetch(j).start()
        if state is not None:
            m_in, acc_in = rest[0], rest[1]
            rest = rest[2:]
        if finish:
            out_ref, m_ref, acc_ref = rest
        else:
            m_ref, acc_ref = rest
        if state is None:
            m_ref[...] = jnp.full(m_ref.shape, NEG, F32)
            acc_ref[...] = jnp.zeros(acc_ref.shape, F32)
        else:
            m_ref[...] = m_in[...]
            acc_ref[...] = acc_in[...]
        me = ep_ref[0]
        base = base_ref[...]
        lane = lax.broadcasted_iota(jnp.int32, (BLOCK, 128), 1)

        def one(j, masked):
            fetch(j).wait()
            kv = kv_ref[j, 0:BLOCK, :]
            parts = kv_ref[j, BLOCK : BLOCK + 32, :].astype(F32)
            gates = (parts[0:8] + parts[8:16]) + parts[16:24]
            decay = base - gates
            row = jnp.concatenate([decay[c : c + 1] for c in range(8)], axis=1)
            values = jnp.where(lane < HEAD, jnp.ones_like(kv), kv)

            def scores(t):
                return nt(q_ref[t * TILE : (t + 1) * TILE, :], kv)

            def update(t, s):
                at = slice(t * TILE, (t + 1) * TILE)
                s = s + row
                if masked:
                    qpos = t * TILE + lax.broadcasted_iota(jnp.int32, (TILE, BLOCK), 0)
                    kpos = lax.broadcasted_iota(jnp.int32, (TILE, BLOCK), 1)
                    s = jnp.where(kpos <= qpos, s, NEG)
                old = m_ref[at, :]
                peak = jnp.maximum(
                    old, jnp.broadcast_to(jnp.max(s, axis=1, keepdims=True), (TILE, 128))
                )
                weight = jnp.exp(s - jnp.concatenate([peak] * (BLOCK // 128), axis=1))
                acc_ref[at, :] = acc_ref[at, :] * jnp.exp(old - peak) + jnp.dot(
                    weight.astype(BF16), values, preferred_element_type=F32
                )
                m_ref[at, :] = peak

            ahead = scores(0)
            for t in range(tiles):
                s = ahead
                if t + 1 < tiles:
                    ahead = scores(t + 1)
                update(t, s)

        def step(j, carry):
            one(j - first, False)
            return carry

        lax.fori_loop(first, jnp.minimum(me, last), step, 0)

        @pl.when((me >= first) & (me < last))
        def _():
            one(me - first, True)

        def drop(j, carry):
            fetch(j - first).wait()
            return carry

        lax.fori_loop(jnp.maximum(jnp.minimum(me + 1, last), first), last, drop, 0)

        if finish:
            for g in range(BLOCK // 64):
                a = acc_ref[64 * g : 64 * g + 32, :]
                b = acc_ref[64 * g + 32 : 64 * g + 64, :]
                pair = [a[:, HEAD:] / a[:, :HEAD], b[:, HEAD:] / b[:, :HEAD]]
                out_ref[32 * g : 32 * g + 32, :] = jnp.concatenate(pair, axis=1).astype(BF16)

    span = last - first
    args = [ep, base, q, *held(kvg)]
    specs = [
        pl.BlockSpec(memory_space=pltpu.SMEM),
        whole(base.shape),
        whole(q.shape),
        pl.BlockSpec(memory_space=pltpu.HBM),
    ]
    wide = jax.ShapeDtypeStruct((BLOCK, 128), F32)
    if state is not None:
        args += list(state)
        specs += [whole(wide.shape)] * 2
    if finish:
        outs = jax.ShapeDtypeStruct((BLOCK // 2, 2 * HEAD), BF16)
        out_specs = whole(outs.shape)
        scratch = [pltpu.VMEM(wide.shape, F32)] * 2
    else:
        outs = (wide, wide)
        out_specs = (whole(wide.shape),) * 2
        scratch = []
    return pl.pallas_call(
        body,
        grid=(1,),
        in_specs=specs,
        out_specs=out_specs,
        out_shape=outs,
        scratch_shapes=scratch
        + [pltpu.VMEM((span,) + kvg.shape[1:], BF16), pltpu.SemaphoreType.DMA((span,))],
        compiler_params=params(),
        name="attend",
        cost_estimate=pl.CostEstimate(
            flops=span * BLOCK * BLOCK * 1024, transcendentals=0, bytes_accessed=4 << 20
        ),
    )(*args)


def arrange(place, low, high, far):
    each = low.shape[0] // HEAD

    def body(place_ref, low_ref, high_ref, far_ref, out_ref):
        chip = lax.div(place_ref[0], 2)
        core = lax.rem(place_ref[0], 2)
        for k in range(2 * each):
            at = jnp.bitwise_xor(chip, k) * 2 * HEAD
            mine = pl.multiple_of(at + core * HEAD, HEAD)
            other = pl.multiple_of(at + (1 - core) * HEAD, HEAD)
            near = low_ref if k < each else high_ref
            piece = slice((k % each) * HEAD, (k % each + 1) * HEAD)
            out_ref[pl.ds(mine, HEAD), :] = near[piece, :]
            out_ref[pl.ds(other, HEAD), :] = far_ref[k * HEAD : (k + 1) * HEAD, :]

    return pl.pallas_call(
        body,
        grid=(1,),
        in_specs=[pl.BlockSpec(memory_space=pltpu.SMEM)]
        + [whole(a.shape) for a in (low, high, far)],
        out_specs=whole((2 * far.shape[0], 128)),
        out_shape=jax.ShapeDtypeStruct((2 * far.shape[0], 128), BF16),
        compiler_params=params(),
        name="arrange",
    )(place, low, high, far)


def project(packed, columns):
    heads, half, _ = packed.shape
    width = heads * HEAD

    def body(a_ref, w_ref, out_ref, rows_ref):
        @pl.when(pl.program_id(0) == 0)
        def _():
            for h in range(0, heads, 2):
                a, b = a_ref[h].astype(F32), a_ref[h + 1].astype(F32)
                at = slice(h * HEAD, (h + 2) * HEAD)
                top = jnp.concatenate([a[:, :HEAD], b[:, :HEAD]], axis=1)
                low = jnp.concatenate([a[:, HEAD:], b[:, HEAD:]], axis=1)
                rows_ref[:half, at] = top.astype(BF16)
                rows_ref[half:, at] = low.astype(BF16)

        both = jnp.concatenate([w_ref[0], w_ref[1]], axis=1)
        out_ref[...] = jnp.dot(rows_ref[...], both, preferred_element_type=F32).astype(BF16)

    return pl.pallas_call(
        body,
        grid=(columns.shape[0] // 2,),
        in_specs=[whole(packed.shape), pl.BlockSpec((2, width, 128), lambda i: (i, 0, 0))],
        out_specs=pl.BlockSpec((2 * half, 256), lambda i: (0, i)),
        out_shape=jax.ShapeDtypeStruct((2 * half, columns.shape[0] * 128), BF16),
        scratch_shapes=[pltpu.VMEM((2 * half, width), BF16)],
        compiler_params=params(),
        name="project",
    )(packed, columns)


def local(
    queries,
    key_vectors,
    value_vectors,
    cumulative_gate,
    out_weight,
    expert_tokens,
    norm_gain,
    gate_weight,
    up_weight,
    down_weight,
    expert_choice,
    route_weights,
):
    n_tp = lax.axis_size("tp")
    n_ep = lax.axis_size("ep")
    chips = n_tp // 2
    d = expert_tokens.shape[1]
    spot = [(z, c) for z in range(chips) for c in range(2)]
    ahead = [(2 * z + c, 2 * ((z + 1 - 2 * c) % chips) + c) for z, c in spot]
    back = [(2 * z + c, 2 * ((z - 1 + 2 * c) % chips) + c) for z, c in spot]
    swap = [(2 * z + c, 2 * z + 1 - c) for z, c in spot]
    fence = lax.optimization_barrier

    def ring(a, b):
        return lax.ppermute(a, "tp", ahead), lax.ppermute(b, "tp", back)

    def across(a, bit):
        return lax.ppermute(a, "tp", [(2 * z + c, 2 * (z ^ bit) + c) for z, c in spot])

    strip = lax.dynamic_slice_in_dim(out_weight, lax.axis_index("ep") * 128, 128, 1)
    strip = jnp.concatenate([strip, across(strip, 1)], axis=0)
    down = down_weight[0]
    da1, db1 = ring(down, down)
    high = lax.reduce_precision(cumulative_gate, 8, 7)
    mid = lax.reduce_precision(cumulative_gate - high, 8, 7)
    low = cumulative_gate - high - mid
    gates = jnp.concatenate([high, mid, low, jnp.zeros_like(low)], axis=1)
    gates = gates.T.reshape(32, 128).astype(BF16)
    packed = jnp.concatenate(
        [jnp.concatenate([key_vectors, value_vectors], axis=1), gates], axis=0
    )
    kvg = lax.all_gather(packed, "ep", axis=0)
    packed, gate_weight, strip = fence((packed, gate_weight, strip))
    strip = jnp.concatenate([strip, across(strip, 2)], axis=0)
    gu = jnp.concatenate([gate_weight, up_weight], axis=0)
    ga1, gb1 = ring(gu, gu)

    gain = norm_gain[None, :]
    outgoing = dispatch(expert_tokens, gain, expert_choice).reshape(n_ep, PAD, d)
    arrived = lax.all_to_all(outgoing, "ep", split_axis=0, concat_axis=0, tiled=True)
    ep = lax.axis_index("ep").astype(jnp.int32).reshape(1)
    strips_high = across(strip, 4)
    q = widen(queries)
    base = jnp.broadcast_to(cumulative_gate[0:1, :], (1, 128))
    da1, db1 = fence((da1, db1))

    da2, db2 = ring(da1, db1)
    ga1, gb1, q, base = fence((ga1, gb1, q, base))

    ga2, gb2 = ring(ga1, gb1)
    far = lax.ppermute(jnp.concatenate([strip, strips_high], axis=0), "tp", swap)
    place = lax.axis_index("tp").astype(jnp.int32).reshape(1)
    strips = arrange(place, strip, strips_high, far)
    columns = lax.all_gather(strips, "ep", axis=0)
    arrived = arrived.reshape(n_ep * PAD, d)
    beside = lax.ppermute(arrived, "tp", swap)
    x = [arrived, beside]
    da2, db2 = fence((da2, db2))

    da3, db3 = ring(da2, db2)
    half = n_ep // 2
    y = experts(x, [gu, ga1, gb1], [down, da1, db1], None)
    state = attend(ep, base, q, kvg, None, 0, half, False)
    ga2, gb2, state = fence((ga2, gb2, state))

    ga3, gb3 = ring(ga2, gb2)
    d4 = lax.ppermute(db3, "tp", back)
    attention = attend(ep, base, q, kvg, state, half, n_ep, True)
    rows = lax.all_to_all(
        attention.reshape(n_tp, -1, 2 * HEAD), "tp", split_axis=0, concat_axis=0, tiled=True
    )
    mixed = mixing(expert_choice, route_weights)
    ga3, gb3, y, attention = fence((ga3, gb3, y, attention))

    g4 = lax.ppermute(ga3, "tp", ahead)
    y = experts(x, [ga2, gb2, ga3, gb3], [da2, db2, da3, db3], y)
    g4, d4, y = fence((g4, d4, y))

    theirs = experts_last(beside, g4, d4, y, arrived.shape[0])
    extra = lax.ppermute(theirs, "tp", swap)
    mine = experts_last(arrived, g4, d4, y, 0)
    results = (mine.astype(F32) + extra.astype(F32)).astype(BF16).reshape(n_ep, PAD, d)
    returned = lax.all_to_all(results, "ep", split_axis=0, concat_axis=0, tiled=True)
    rows, results = fence((rows, results))
    mixer_output = project(rows, columns)
    expert_output = combine(returned.reshape(n_ep * PAD, d), *mixed)
    return (mixer_output, expert_output)


def solution(mesh):
    placed = (
        P("ep", "tp"),
        P("ep", "tp"),
        P("ep", "tp"),
        P("ep", "tp"),
        P("tp", None),
        P(("ep", "tp"), None),
        P(),
        P("ep", None, "tp"),
        P("ep", None, "tp"),
        P("ep", "tp", None),
        P(("ep", "tp"), None),
        P(("ep", "tp"), None),
    )

    return jax.shard_map(
        local,
        mesh=mesh,
        in_specs=placed,
        out_specs=(P(("ep", "tp"), None), P(("ep", "tp"), None)),
        check_vma=False,
    )
```
